32 devices in a mesh: fs: 8 (over z, y), tp: 4 (over x, core).
Axes of the slice: x: 2, y: 2, z: 4, core: 2. Of those that a mesh axis runs over, the one named last changes fastest.
Arguments:
- tokens: bfloat16 [8192, 2048], P('fs', 'tp'), may hold values from -6 to 6
- mixer_gain: float32 [2048], replicated, may hold values from 0.1 to 1.9
- ffn_gain: float32 [2048], replicated, may hold values from 0.1 to 1.9
- w_outer: float32 [2048, 1024], P('fs', 'tp'), may hold values from -0.125 to 0.125
- w_inner: float32 [2048, 1024], P('fs', 'tp'), may hold values from -0.125 to 0.125
- w_value: float32 [2048, 1024], P('fs', 'tp'), may hold values from -0.125 to 0.125
- scale_outer: float32 [1, 1024], P(None, 'tp'), may hold values from 0.5 to 2
- scale_inner: float32 [1, 1024], P(None, 'tp'), may hold values from 0.5 to 2
- scale_value: float32 [1, 1024], P(None, 'tp'), may hold values from 0.5 to 2
- conv_taps: float32 [3, 1024], P(None, 'tp'), may hold values from -3.5 to 3.5
- w_mixout: float32 [1024, 2048], P('tp', 'fs'), may hold values from -0.1875 to 0.1875
- scale_mixout: float32 [1, 2048], P(None, 'fs'), may hold values from 0.5 to 2
- w_gate: float32 [2048, 5632], P('fs', 'tp'), may hold values from -0.125 to 0.125
- w_upward: float32 [2048, 5632], P('fs', 'tp'), may hold values from -0.125 to 0.125
- scale_gate: float32 [1, 5632], P(None, 'tp'), may hold values from 0.5 to 2
- scale_upward: float32 [1, 5632], P(None, 'tp'), may hold values from 0.5 to 2
- w_down: float32 [5632, 2048], P('tp', 'fs'), may hold values from -0.078125 to 0.078125
- scale_down: float32 [1, 2048], P(None, 'fs'), may hold values from 0.5 to 2
Outputs:
- block_out: bfloat16 [8192, 2048], P('fs', 'tp')
The draws below stay inside these ranges and needn't reach their ends.
All inputs are finite; a program needn't handle non-finite values.
Results may differ from the reference program's by a relative error of at most 0.019.
Values may be sent and summed in bfloat16 or wider, within the bound.
No kernel may reach another device: no remote copies, remote signals or barrier semaphores. Data moves between devices by JAX's collectives and lax.ppermute only.
A program may use at most 128 MiB of HBM per device.

```python
import math
import jax
import jax.numpy as jnp
from jax import lax

MODEL = 2048
CHANNELS = 1024
HIDDEN_SIZE = 5632
TAPS = 3
SEQ_LEN = 128
TOKENS = 8192
N_TP = 4


def levels(rng, extent, pieces, low, high):
    def one(position, blocks):
        draws = jax.random.uniform(jax.random.fold_in(jax.random.fold_in(rng, 6), position), (blocks,), jnp.float32, low / len(pieces), high / len(pieces))
        return jnp.repeat(jnp.exp(draws), extent[position] // blocks).reshape((-1,) + (1,) * (len(extent) - position - 1))

    factor_of = one(*pieces[0])
    for cut in pieces[1:]:
        factor_of = factor_of * one(*cut)
    return factor_of


def scatter_about(rng, dims, deviation, reach, pieces=(), kind=jnp.bfloat16):
    result = jax.random.normal(rng, dims, jnp.float32) * deviation
    if len(pieces) > 0:
        result = levels(rng, dims, pieces, -0.22, 0.18) * result
    return jnp.clip(result, min=-reach, max=reach).astype(kind)


def setup_inputs(seed: int = 0) -> dict:
    splits = jax.random.split(jax.random.key(seed), 19)
    return {
        "tokens": scatter_about(splits[0], (TOKENS, MODEL), 1.0, 6.0, ((0, 8), (1, 4))),
        "mixer_gain": jnp.clip(1.0 + 0.18 * jax.random.normal(splits[1], (MODEL,), jnp.float32), 0.1, 1.9),
        "ffn_gain": jnp.clip(1.0 + 0.18 * jax.random.normal(splits[2], (MODEL,), jnp.float32), 0.1, 1.9),
        "w_outer": scatter_about(splits[3], (MODEL, CHANNELS), MODEL ** -0.5, 0.125, ((0, 8), (1, 4)), jnp.float32),
        "w_inner": scatter_about(splits[4], (MODEL, CHANNELS), MODEL ** -0.5, 0.125, ((0, 8), (1, 4)), jnp.float32),
        "w_value": scatter_about(splits[5], (MODEL, CHANNELS), MODEL ** -0.5, 0.125, ((0, 8), (1, 4)), jnp.float32),
        "scale_outer": jnp.clip(jnp.exp(math.log(2.0) - 1.3862944 * jax.random.uniform(splits[6], (1, CHANNELS), jnp.float32) ** levels(splits[6], (1, CHANNELS), ((1, 4),), -0.2, 0.2)), 0.5, 2.0),
        "scale_inner": jnp.clip(jnp.exp(math.log(2.0) - 1.3862944 * jax.random.uniform(splits[7], (1, CHANNELS), jnp.float32) ** levels(splits[7], (1, CHANNELS), ((1, 4),), -0.2, 0.2)), 0.5, 2.0),
        "scale_value": jnp.clip(jnp.exp(math.log(2.0) - 1.3862944 * jax.random.uniform(splits[8], (1, CHANNELS), jnp.float32) ** levels(splits[8], (1, CHANNELS), ((1, 4),), -0.2, 0.2)), 0.5, 2.0),
        "conv_taps": scatter_about(splits[9], (TAPS, CHANNELS), TAPS ** -0.5, 3.5, ((1, 4),), jnp.float32),
        "w_mixout": scatter_about(splits[10], (CHANNELS, MODEL), CHANNELS ** -0.5, 0.1875, ((0, 4), (1, 8)), jnp.float32),
        "scale_mixout": jnp.clip(jnp.exp(math.log(2.0) - 1.3862944 * jax.random.uniform(splits[11], (1, MODEL), jnp.float32) ** levels(splits[11], (1, MODEL), ((1, 8),), -0.2, 0.2)), 0.5, 2.0),
        "w_gate": scatter_about(splits[12], (MODEL, HIDDEN_SIZE), MODEL ** -0.5, 0.125, ((0, 8), (1, 4)), jnp.float32),
        "w_upward": scatter_about(splits[13], (MODEL, HIDDEN_SIZE), MODEL ** -0.5, 0.125, ((0, 8), (1, 4)), jnp.float32),
        "scale_gate": jnp.clip(jnp.exp(math.log(2.0) - 1.3862944 * jax.random.uniform(splits[14], (1, HIDDEN_SIZE), jnp.float32) ** levels(splits[14], (1, HIDDEN_SIZE), ((1, 4),), -0.2, 0.2)), 0.5, 2.0),
        "scale_upward": jnp.clip(jnp.exp(math.log(2.0) - 1.3862944 * jax.random.uniform(splits[15], (1, HIDDEN_SIZE), jnp.float32) ** levels(splits[15], (1, HIDDEN_SIZE), ((1, 4),), -0.2, 0.2)), 0.5, 2.0),
        "w_down": scatter_about(splits[16], (HIDDEN_SIZE, MODEL), HIDDEN_SIZE ** -0.5, 0.078125, ((0, 4), (1, 8)), jnp.float32),
        "scale_down": jnp.clip(jnp.exp(math.log(2.0) - 1.3862944 * jax.random.uniform(splits[17], (1, MODEL), jnp.float32) ** levels(splits[17], (1, MODEL), ((1, 8),), -0.2, 0.2)), 0.5, 2.0),
    }


def rms_scaled(full_rows, gain_vec):
    values = full_rows.astype(jnp.float32)
    inverse = lax.rsqrt(lax.optimization_barrier(jnp.mean(values * values, axis=-1, keepdims=True)) + 1e-06)
    return (values * inverse * gain_vec).astype(jnp.bfloat16)

def causal_taps(product, conv_taps):
    padded = jnp.pad(product, ((0, 0), (TAPS - 1, 0), (0, 0)))
    length = product.shape[1]
    summed = jnp.zeros(product.shape, jnp.float32)
    for tap_index in range(TAPS):
        summed = summed + conv_taps[tap_index] * padded[:, tap_index:tap_index + length, :]
    return summed

def reference(tokens, mixer_gain, ffn_gain, w_outer, w_inner, w_value, scale_outer, scale_inner, scale_value, conv_taps, w_mixout, scale_mixout, w_gate, w_upward, scale_gate, scale_upward, w_down, scale_down):
    normed = rms_scaled(tokens, mixer_gain)

    def project(weight, column_scale):
        return jnp.dot(normed, weight.astype(jnp.bfloat16), preferred_element_type=jnp.float32) * column_scale
    outer = project(w_outer, scale_outer)
    inner = project(w_inner, scale_inner)
    value = project(w_value, scale_value)
    product = (inner * value).reshape(-1, SEQ_LEN, CHANNELS)
    conv = causal_taps(product, conv_taps).reshape(-1, CHANNELS)
    mixed_out = (outer * conv).astype(jnp.bfloat16)
    mix_term = jnp.dot(mixed_out, w_mixout.astype(jnp.bfloat16), preferred_element_type=jnp.float32) * scale_mixout
    residual = (tokens.astype(jnp.float32) + mix_term).astype(jnp.bfloat16)
    normed_ffn = rms_scaled(residual, ffn_gain)
    gate_proj = jnp.dot(normed_ffn, w_gate.astype(jnp.bfloat16), preferred_element_type=jnp.float32) * scale_gate
    up_proj = jnp.dot(normed_ffn, w_upward.astype(jnp.bfloat16), preferred_element_type=jnp.float32) * scale_upward
    hidden = (jax.nn.silu(gate_proj) * up_proj).astype(jnp.bfloat16)
    down_bf = w_down.astype(jnp.bfloat16)
    block_width = HIDDEN_SIZE // N_TP

    def add_block(summed, block_index):
        offset = (block_index * block_width).astype(jnp.int32)
        left = lax.dynamic_slice_in_dim(hidden, offset, block_width, 1)
        right = lax.dynamic_slice_in_dim(down_bf, offset, block_width, 0)
        part = (jnp.dot(left, right, preferred_element_type=jnp.float32) * scale_down).astype(jnp.bfloat16)
        part = lax.optimization_barrier(part)
        return (summed + part.astype(jnp.float32), None)
    ffn_sum, _ = lax.scan(add_block, jnp.zeros(residual.shape, jnp.float32), jnp.arange(N_TP, dtype=jnp.int32))
    return (residual.astype(jnp.float32) + ffn_sum).astype(jnp.bfloat16)
```

```python
import jax
import jax.numpy as jnp
from jax import lax
from jax.sharding import PartitionSpec as P

SEQ_LEN = 128


def rms_scaled(full_rows, gain_vec):
    values = full_rows.astype(jnp.float32)
    inverse = lax.rsqrt(jnp.mean(values * values, axis=-1, keepdims=True) + 1e-06)
    return (values * inverse * gain_vec).astype(jnp.bfloat16)


def add_rows(left, w_piece):
    return jnp.dot(left, w_piece, preferred_element_type=jnp.float32)


def causal_taps(product, conv_taps):
    padded = jnp.pad(product, ((0, 0), (conv_taps.shape[0] - 1, 0), (0, 0)))
    length = product.shape[1]
    summed = jnp.zeros(product.shape, jnp.float32)
    for tap_index in range(conv_taps.shape[0]):
        summed = summed + conv_taps[tap_index] * padded[:, tap_index : tap_index + length, :]
    return summed


RING = []


def grid_ring(mesh):
    count = mesh.shape["fs"]
    axis = mesh.axis_names.index("fs")
    line = [mesh.devices.take(i, axis=axis).flat[0] for i in range(count)]
    spots = [tuple(getattr(d, "coords", (0, 0, i)))[1:] for i, d in enumerate(line)]
    where = {spot: i for i, spot in enumerate(spots)}
    ys = sorted({spot[0] for spot in spots})
    zs = sorted({spot[1] for spot in spots})
    if len(where) != count or len(ys) * len(zs) != count or len(ys) < 2 or len(zs) % 2:
        return list(range(count))
    order = [where[(ys[0], z)] for z in zs]
    for step, z in enumerate(reversed(zs)):
        rest = ys[1:] if step % 2 == 0 else ys[:0:-1]
        order += [where[(y, z)] for y in rest]
    return order


def ring_gather(shard, axis, flip):
    count = len(RING)
    table = jnp.array(RING, jnp.int32)
    mine = lax.axis_index("fs")
    spot = jnp.argmax(table == mine).astype(jnp.int32)
    up = [(RING[i], RING[(i + 1) % count]) for i in range(count)]
    down = [(dst, src) for src, dst in up]
    ways = [(up, -1, count // 2), (down, 1, count - 1 - count // 2)]
    if flip:
        ways = [(down, 1, count // 2), (up, -1, count - 1 - count // 2)]
    shape = list(shard.shape)
    size = shape[axis]
    shape[axis] = size * count
    whole = lax.dynamic_update_slice_in_dim(
        jnp.zeros(tuple(shape), shard.dtype), shard, mine * size, axis
    )
    pieces = []
    held = [shard, shard]
    for step in range(1, count // 2 + 1):
        for way, (pairs, sign, hops) in enumerate(ways):
            if step <= hops:
                held[way] = lax.ppermute(held[way], "fs", pairs)
                pieces.append((held[way], table[(spot + sign * step) % count]))
    for piece, owner in pieces:
        whole = lax.dynamic_update_slice_in_dim(whole, piece, owner * size, axis)
    return whole


def three_parts(values):
    parts = []
    rest = values
    for _ in range(3):
        part = lax.reduce_precision(rest, 8, 7)
        parts.append(part.astype(jnp.bfloat16))
        rest = rest - part
    return parts


def per_device(
    tokens,
    mixer_gain,
    ffn_gain,
    w_outer,
    w_inner,
    w_value,
    scale_outer,
    scale_inner,
    scale_value,
    conv_taps,
    w_mixout,
    scale_mixout,
    w_gate,
    w_upward,
    scale_gate,
    scale_upward,
    w_down,
    scale_down,
):
    bf = jnp.bfloat16
    f32 = jnp.float32
    tok_count, feature_count = tokens.shape
    local_channels = w_outer.shape[1]
    count = len(RING)
    full_rows = lax.all_gather(tokens, "tp", axis=1, tiled=True)

    mixer_shard = jnp.concatenate([w_inner.astype(bf), w_value.astype(bf), w_outer.astype(bf)], 1)
    out_cols = scale_mixout.shape[1]
    scale_rows = jnp.concatenate(
        three_parts(scale_mixout) + three_parts(scale_down) + [jnp.zeros((10, out_cols), bf)], 0
    )
    mixout_shard = jnp.concatenate([w_mixout.astype(bf), scale_rows], 0)
    mixer_all = ring_gather(mixer_shard, 0, False)
    mixout_cols = ring_gather(mixout_shard, 1, True)
    gate_all = ring_gather(w_gate.astype(bf), 0, False)
    up_all = ring_gather(w_upward.astype(bf), 0, True)
    down_all = ring_gather(w_down.astype(bf), 1, False)

    normed = rms_scaled(full_rows, mixer_gain)
    projected = add_rows(normed, mixer_all)
    inner = projected[:, :local_channels] * scale_inner
    value = projected[:, local_channels : 2 * local_channels] * scale_value
    outer = projected[:, 2 * local_channels :] * scale_outer
    product = (inner * value).reshape(tok_count // SEQ_LEN, SEQ_LEN, local_channels)
    conv = causal_taps(product, conv_taps).reshape(tok_count, local_channels)
    mixed_out = (outer * conv).astype(bf)
    mixed_all = lax.all_gather(mixed_out, "tp", axis=1, tiled=True)
    scales = mixout_cols[local_channels:].astype(f32)
    mixout_scales = (scales[0:1] + scales[1:2]) + scales[2:3]
    down_scales = (scales[3:4] + scales[4:5]) + scales[5:6]
    mixout_all = lax.all_gather(mixout_cols[:local_channels], "tp", axis=0, tiled=True)
    mix_term = jnp.dot(mixed_all, mixout_all, preferred_element_type=f32) * mixout_scales
    residual_rows = (full_rows.astype(f32) + mix_term).astype(bf)
    place = lax.axis_index("tp")
    residual = lax.dynamic_slice_in_dim(residual_rows, place * feature_count, feature_count, 1)
    normed_ffn = rms_scaled(residual_rows, ffn_gain)
    gate_proj = add_rows(normed_ffn, gate_all)
    up_proj = add_rows(normed_ffn, up_all)
    hidden = (jax.nn.silu(gate_proj * scale_gate) * (up_proj * scale_upward)).astype(bf)

    tp_count = lax.axis_size("tp")
    halves = tp_count // 2
    swap_core = [(i, i ^ 1) for i in range(tp_count)]
    chip = place // 2
    core = place % 2

    def part(block):
        first = block * feature_count
        w_cols = lax.dynamic_slice_in_dim(down_all, first, feature_count, 1)
        s_cols = lax.dynamic_slice_in_dim(down_scales, first, feature_count, 1)
        return jnp.dot(hidden, w_cols, preferred_element_type=f32) * s_cols

    total = None
    for hop in range(1, halves + 1):
        target = (chip + hop) % halves
        theirs = lax.ppermute(part(2 * target + 1 - core).astype(bf), "tp", swap_core)
        pair_sum = part(2 * target + core).astype(bf).astype(f32) + theirs.astype(f32)
        if hop < halves:
            to_chip = [(i, (i + 2 * hop) % tp_count) for i in range(tp_count)]
            pair_sum = lax.ppermute(pair_sum.astype(bf), "tp", to_chip).astype(f32)
        total = pair_sum if total is None else total + pair_sum
    return (residual.astype(f32) + total).astype(bf)


def solution(mesh):
    RING[:] = grid_ring(mesh)
    in_specs = (
        P("fs", "tp"),
        P(),
        P(),
        P("fs", "tp"),
        P("fs", "tp"),
        P("fs", "tp"),
        P(None, "tp"),
        P(None, "tp"),
        P(None, "tp"),
        P(None, "tp"),
        P("tp", "fs"),
        P(None, "fs"),
        P("fs", "tp"),
        P("fs", "tp"),
        P(None, "tp"),
        P(None, "tp"),
        P("tp", "fs"),
        P(None, "fs"),
    )
    out_specs = P("fs", "tp")
    return jax.shard_map(
        per_device, mesh=mesh, in_specs=in_specs, out_specs=out_specs, check_vma=False
    )
```

```python
import jax
import jax.numpy as jnp
from jax import lax
from jax.sharding import PartitionSpec as P

SEQ_LEN = 128


def rms_scaled(full_rows, gain_vec):
    values = full_rows.astype(jnp.float32)
    inverse = lax.rsqrt(jnp.mean(values * values, axis=-1, keepdims=True) + 1e-06)
    return (values * inverse * gain_vec).astype(jnp.bfloat16)


def add_rows(left, w_piece):
    return jnp.dot(left, w_piece, preferred_element_type=jnp.float32)


def causal_taps(product, conv_taps):
    padded = jnp.pad(product, ((0, 0), (conv_taps.shape[0] - 1, 0), (0, 0)))
    length = product.shape[1]
    summed = jnp.zeros(product.shape, jnp.float32)
    for tap_index in range(conv_taps.shape[0]):
        summed = summed + conv_taps[tap_index] * padded[:, tap_index : tap_index + length, :]
    return summed


RING = []


def grid_ring(mesh):
    count = mesh.shape["fs"]
    axis = mesh.axis_names.index("fs")
    line = [mesh.devices.take(i, axis=axis).flat[0] for i in range(count)]
    spots = [tuple(getattr(d, "coords", (0, 0, i)))[1:] for i, d in enumerate(line)]
    where = {spot: i for i, spot in enumerate(spots)}
    ys = sorted({spot[0] for spot in spots})
    zs = sorted({spot[1] for spot in spots})
    if len(where) != count or len(ys) * len(zs) != count or len(ys) < 2 or len(zs) % 2:
        return list(range(count))
    order = [where[(ys[0], z)] for z in zs]
    for step, z in enumerate(reversed(zs)):
        rest = ys[1:] if step % 2 == 0 else ys[:0:-1]
        order += [where[(y, z)] for y in rest]
    return order


class Ring:
    def __init__(self, shard, axis, flip):
        count = len(RING)
        self.shard, self.axis, self.count = lax.optimization_barrier(shard), axis, count
        self.table = jnp.array(RING, jnp.int32)
        self.mine = lax.axis_index("fs")
        places = [0] * count
        for i, owner in enumerate(RING):
            places[owner] = i
        self.spot = jnp.array(places, jnp.int32)[self.mine]
        up = [(RING[i], RING[(i + 1) % count]) for i in range(count)]
        down = [(dst, src) for src, dst in up]
        first, last = ((down, 1), (up, -1)) if flip else ((up, -1), (down, 1))
        self.ways = [first + (count // 2,), last + (count - 1 - count // 2,)]
        self.held = [self.shard, self.shard]
        self.pieces = [(self.shard, self.mine)]

    def step(self, hop, gate):
        arrived = []
        for way, (pairs, sign, hops) in enumerate(self.ways):
            if hop <= hops:
                sent = self.held[way]
                if gate:
                    sent = lax.optimization_barrier((sent, *gate))[0]
                self.held[way] = lax.ppermute(sent, "fs", pairs)
                owner = self.table[(self.spot + sign * hop) % self.count]
                self.pieces.append((self.held[way], owner))
                arrived.append(self.held[way])
        return arrived

    def whole(self):
        shape = list(self.shard.shape)
        size = shape[self.axis]
        shape[self.axis] = size * self.count
        out = jnp.zeros(tuple(shape), self.shard.dtype)
        for piece, owner in self.pieces:
            out = lax.dynamic_update_slice_in_dim(out, piece, owner * size, self.axis)
        return out


def run_rings(mixer, gate_up, down, mix, residue, gating, hiding):
    hops = len(RING) // 2
    mixes = [[(ring, hop) for ring in mixer] for hop in range(1, hops + 1)]
    wide = [[(ring, hop)] for hop in range(1, hops) for ring in gate_up]
    last = [(ring, hops) for ring in gate_up]
    early, late = ([[(ring, hop)] for hop in range(1, hops + 1)] for ring in down)
    order = []
    for i in range(max(len(mixes), len(wide))):
        order += mixes[i : i + 1] + wide[i : i + 1]
    order += early[:1] + [last]
    for i in range(1, hops + 1):
        order += early[i : i + 1] + late[i - 1 : i]
    wide_end = order.index(last)
    work = {order.index(mixes[-1]) + 3: mix, wide_end: residue}
    work.update({wide_end + 4: gating, wide_end + 6: hiding})
    arrivals = []
    for i, group in enumerate(order):
        gate = list(arrivals[i - 3]) if i >= 3 else []
        if i in work:
            gate.append(work[i]())
        arrivals.append([got for ring, hop in group for got in ring.step(hop, gate)])


def three_parts(values):
    parts = []
    rest = values
    for _ in range(3):
        part = lax.reduce_precision(rest, 8, 7)
        parts.append(part.astype(jnp.bfloat16))
        rest = rest - part
    return parts


def per_device(
    tokens,
    mixer_gain,
    ffn_gain,
    w_outer,
    w_inner,
    w_value,
    scale_outer,
    scale_inner,
    scale_value,
    conv_taps,
    w_mixout,
    scale_mixout,
    w_gate,
    w_upward,
    scale_gate,
    scale_upward,
    w_down,
    scale_down,
):
    bf = jnp.bfloat16
    f32 = jnp.float32
    tok_count, feature_count = tokens.shape
    local_channels = w_outer.shape[1]
    count = len(RING)
    full_rows = lax.all_gather(tokens, "tp", axis=1, tiled=True)

    mixer_shard = jnp.concatenate([w_inner.astype(bf), w_value.astype(bf), w_outer.astype(bf)], 1)
    out_cols = scale_mixout.shape[1]
    scale_rows = jnp.concatenate(
        three_parts(scale_mixout) + three_parts(scale_down) + [jnp.zeros((10, out_cols), bf)], 0
    )
    mixout_shard = jnp.concatenate([w_mixout.astype(bf), scale_rows], 0)
    half = out_cols // 2
    down_shard = w_down.astype(bf)
    rings = [
        Ring(mixer_shard, 0, False),
        Ring(mixout_shard, 1, True),
        Ring(w_gate.astype(bf), 0, False),
        Ring(w_upward.astype(bf), 0, True),
        Ring(down_shard[:, :half], 1, False),
        Ring(down_shard[:, half:], 1, True),
    ]
    place = lax.axis_index("tp")
    done = {}

    def mix():
        projected = add_rows(rms_scaled(full_rows, mixer_gain), rings[0].whole())
        inner = projected[:, :local_channels] * scale_inner
        value = projected[:, local_channels : 2 * local_channels] * scale_value
        outer = projected[:, 2 * local_channels :] * scale_outer
        product = (inner * value).reshape(tok_count // SEQ_LEN, SEQ_LEN, local_channels)
        conv = causal_taps(product, conv_taps).reshape(tok_count, local_channels)
        done["mixed"] = (outer * conv).astype(bf)
        return done["mixed"]

    def residue():
        mixout_cols = rings[1].whole()
        mixed_all = lax.all_gather(done["mixed"], "tp", axis=1, tiled=True)
        scales = mixout_cols[local_channels:].astype(f32)
        mixout_scales = (scales[0:1] + scales[1:2]) + scales[2:3]
        done["scales"] = (scales[3:4] + scales[4:5]) + scales[5:6]
        mixout_all = lax.all_gather(mixout_cols[:local_channels], "tp", axis=0, tiled=True)
        mix_term = jnp.dot(mixed_all, mixout_all, preferred_element_type=f32) * mixout_scales
        done["residual"] = (full_rows.astype(f32) + mix_term).astype(bf)
        return done["residual"]

    def gating():
        done["normed"] = rms_scaled(done["residual"], ffn_gain)
        done["gate"] = add_rows(done["normed"], rings[2].whole())
        return done["gate"]

    def hiding():
        up_proj = add_rows(done["normed"], rings[3].whole())
        gated = jax.nn.silu(done["gate"] * scale_gate)
        done["hidden"] = (gated * (up_proj * scale_upward)).astype(bf)
        return done["hidden"]

    run_rings(rings[:2], rings[2:4], rings[4:], mix, residue, gating, hiding)
    down_early, down_late = rings[4].whole(), rings[5].whole()
    down_scales, hidden = done["scales"], done["hidden"]
    residual = lax.dynamic_slice_in_dim(
        done["residual"], place * feature_count, feature_count, 1
    )

    tp_count = lax.axis_size("tp")
    halves = tp_count // 2
    swap_core = [(i, i ^ 1) for i in range(tp_count)]
    chip = place // 2
    core = place % 2

    shards = count // tp_count
    by_shard = down_scales.reshape(1, count, 2, half)

    def shares(down_half, which):
        scale_half = by_shard[:, :, which].reshape(1, count * half)
        width = shards * half

        def part(block):
            w_cols = lax.dynamic_slice_in_dim(down_half, block * width, width, 1)
            s_cols = lax.dynamic_slice_in_dim(scale_half, block * width, width, 1)
            return jnp.dot(hidden, w_cols, preferred_element_type=f32) * s_cols

        total = None
        for hop in range(1, halves + 1):
            target = (chip + hop) % halves
            theirs = lax.ppermute(part(2 * target + 1 - core).astype(bf), "tp", swap_core)
            pair_sum = part(2 * target + core).astype(bf).astype(f32) + theirs.astype(f32)
            if hop < halves:
                to_chip = [(i, (i + 2 * hop) % tp_count) for i in range(tp_count)]
                pair_sum = lax.ppermute(pair_sum.astype(bf), "tp", to_chip).astype(f32)
            total = pair_sum if total is None else total + pair_sum
        return total

    early, late = shares(down_early, 0), shares(down_late, 1)
    columns = []
    for i in range(shards):
        columns += [early[:, i * half : (i + 1) * half], late[:, i * half : (i + 1) * half]]
    total = jnp.concatenate(columns, 1)
    return (residual.astype(f32) + total).astype(bf)


def solution(mesh):
    RING[:] = grid_ring(mesh)
    in_specs = (
        P("fs", "tp"),
        P(),
        P(),
        P("fs", "tp"),
        P("fs", "tp"),
        P("fs", "tp"),
        P(None, "tp"),
        P(None, "tp"),
        P(None, "tp"),
        P(None, "tp"),
        P("tp", "fs"),
        P(None, "fs"),
        P("fs", "tp"),
        P("fs", "tp"),
        P(None, "tp"),
        P(None, "tp"),
        P("tp", "fs"),
        P(None, "fs"),
    )
    out_specs = P("fs", "tp")
    return jax.shard_map(
        per_device, mesh=mesh, in_specs=in_specs, out_specs=out_specs, check_vma=False
    )
```
